512 devices in a mesh: grp: 2 (over y), ep: 64 (over z, core), tp: 4 (over x).
Axes of the slice: x: 4, y: 2, z: 32, core: 2. Of those that a mesh axis runs over, the one named last changes fastest.
The devices are a block of a 4x8x32 slice.
Arguments:
- tokens: bfloat16 [49152, 2048], P(('grp', 'ep'), 'tp'), parts along dimension 0
- group_choice: int32 [49152], P(('grp', 'ep')), parts along dimension 0, may hold values from 0 to 7, as said below
- expert_choice: int32 [49152, 2], P(('grp', 'ep')), parts along dimension 0, may hold values from 0 to 7, as said below
- group_weight: float32 [49152], P(('grp', 'ep')), parts along dimension 0, may hold values from 0.3 to 1
- expert_weight: float32 [49152, 2], P(('grp', 'ep')), parts along dimension 0, may hold values from 0.1 to 1
- norm_gain: float32 [2048], replicated, may hold values from 0.1 to 1.9
- w_gate: bfloat16 [64, 2048, 1024], P('ep', None, 'tp'), may hold values from -0.125 to 0.125
- w_up: bfloat16 [64, 2048, 1024], P('ep', None, 'tp'), may hold values from -0.125 to 0.125
- w_down: bfloat16 [64, 1024, 2048], P('ep', None, 'tp'), may hold values from -0.1875 to 0.1875
Outputs:
- moe_out: bfloat16 [49152, 2048], P(('grp', 'ep'), 'tp'), parts along dimension 0
The draws below stay inside these ranges and needn't reach their ends.
There are 2 independent parts, one for each index of `grp`. The reference program is written for one: setup_inputs(seed, part) draws one part's arguments, and reference() takes and returns one part's arrays. A program takes and returns all parts, laid end to end along the dimension named above; an argument that names none is the same for every part. Nothing has to cross between parts.
Inputs may be any that keep to these rules, and one draw needn't show every extreme that they name: `group_choice`: group of each token, 0 to 7; within each aligned block of 384 tokens (the tokens of one index of ep) every group is chosen by the same number of tokens. `expert_choice`: a token's two entries differ; within each aligned block of 384 tokens no expert (group with entry) is named by more than 18 tokens, and in every block one expert of each group, the same one in all blocks, is named by exactly 18 tokens.
All inputs are finite; a program needn't handle non-finite values.
Results may differ from the reference program's by a relative error of at most 0.0071.
Values may be sent and summed in bfloat16 or wider, within the bound.
A program may use at most 64 MiB of HBM per device.

```python
import math
import jax
import jax.numpy as jnp
from jax import lax

D = 2048
FF = 1024
TOK_DEV = 384
TOP_K = 2
EXPERTS = 64
EXPERTS_GROUP = 8
GROUPS = 8
CAP = 18
TOKENS = 24576


def route_tables(key):
    base = jax.random.fold_in(key, 11)
    per_group = TOK_DEV // GROUPS
    mean_load = 2 * per_group // EXPERTS_GROUP
    swing = min(mean_load // 2, per_group - mean_load)
    pairs = EXPERTS_GROUP // 2
    blocks = TOKENS // TOK_DEV
    order_keys = jax.random.split(jax.random.fold_in(base, 1), GROUPS)
    orders = jax.vmap(lambda one_key: jax.random.permutation(one_key, EXPERTS_GROUP))(order_keys)

    def one_block(block_key):
        key_shift, key_seat, key_flip = jax.random.split(block_key, 3)
        shifts = jax.random.randint(key_shift, (GROUPS, pairs), -swing, swing + 1)
        shifts = shifts.at[:, 0].set(swing)
        loads = jnp.stack([mean_load + shifts, mean_load - shifts], -1).reshape(GROUPS, EXPERTS_GROUP)
        placed = jnp.zeros((GROUPS, EXPERTS_GROUP), jnp.int32).at[jnp.arange(GROUPS)[:, None], orders].set(loads.astype(jnp.int32))
        ends = jnp.cumsum(placed, -1)
        spots = jnp.arange(2 * per_group, dtype=jnp.int32)
        labels = jnp.sum((spots[None, :, None] >= ends[:, None, :]).astype(jnp.int32), -1)
        first = labels[:, :per_group].reshape(-1)
        second = labels[:, per_group:].reshape(-1)
        flips = jax.random.randint(key_flip, (TOK_DEV,), 0, 2)
        first_swapped = jnp.where(flips == 1, second, first)
        second_swapped = jnp.where(flips == 1, first, second)
        seats = jax.random.permutation(key_seat, TOK_DEV)
        group_rank = (jnp.arange(TOK_DEV, dtype=jnp.int32) // per_group).astype(jnp.int32)
        group_of = jnp.zeros((TOK_DEV,), jnp.int32).at[seats].set(group_rank)
        first_of = jnp.zeros((TOK_DEV,), jnp.int32).at[seats].set(first_swapped)
        second_of = jnp.zeros((TOK_DEV,), jnp.int32).at[seats].set(second_swapped)
        return (group_of, jnp.stack([first_of, second_of], -1))
    block_keys = jax.random.split(jax.random.fold_in(base, 2), blocks)
    groups_all, experts_all = jax.vmap(one_block)(block_keys)
    return (groups_all.reshape(TOKENS), experts_all.reshape(TOKENS, TOP_K))


def draw_group_choice(key, part):
    return route_tables(key)[0]


def draw_expert_choice(key, part):
    return route_tables(key)[1]


def draw_tokens(key, part):
    key_main = jax.random.fold_in(jax.random.fold_in(key, 5), 0)
    column_scale = jnp.exp(math.log(4.0) * jnp.arange(D, dtype=jnp.float32) / D)
    values = jax.random.normal(key_main, (TOKENS, D), jnp.float32)
    return (values * column_scale[None, :]).astype(jnp.bfloat16)


def shard_levels(rng, shape, pieces, low, top_value):
    gain = 1.0
    for axis_at, parts in pieces:
        steps = jax.random.uniform(jax.random.fold_in(jax.random.fold_in(rng, 6), axis_at), (parts,), jnp.float32, low / len(pieces), top_value / len(pieces))
        gain = gain * jnp.repeat(jnp.exp(steps), shape[axis_at] // parts).reshape((-1,) + (1,) * (len(shape) - 1 - axis_at))
    return gain


def bell_draw(own_key, shape, deviation, most, cuts=(), held_as=jnp.bfloat16):
    values = deviation * jax.random.normal(own_key, shape, jnp.float32)
    if cuts:
        values = values * shard_levels(own_key, shape, cuts, -0.22, 0.18)
    return jnp.clip(values, -most, most).astype(held_as)


def setup_inputs(seed: int = 0, part: int = 0) -> dict:
    key_list = jax.random.split(jax.random.key(seed), 10)
    part_splits = jax.random.split(jax.random.fold_in(key_list[9], part), 10)
    return {
        "tokens": draw_tokens(jax.random.fold_in(jax.random.fold_in(key_list[9], part), 71), part),
        "group_choice": draw_group_choice(jax.random.fold_in(jax.random.fold_in(key_list[9], part), 71), part),
        "expert_choice": draw_expert_choice(jax.random.fold_in(jax.random.fold_in(key_list[9], part), 71), part),
        "group_weight": jnp.clip(0.3 + 0.7 * jax.random.uniform(part_splits[3], (TOKENS,), jnp.float32) ** shard_levels(part_splits[3], (TOKENS,), ((0, 64),), -0.2, 0.2), 0.3, 1.0),
        "expert_weight": jnp.clip(jnp.exp(math.log(1.0) - 2.3025851 * jax.random.uniform(part_splits[4], (TOKENS, TOP_K), jnp.float32) ** shard_levels(part_splits[4], (TOKENS, TOP_K), ((0, 64),), -0.2, 0.2)), 0.1, 1.0),
        "norm_gain": jnp.clip(1.0 + 0.18 * jax.random.normal(key_list[5], (D,), jnp.float32), 0.1, 1.9),
        "w_gate": bell_draw(key_list[6], (EXPERTS, D, FF), D ** -0.5, 0.125, ((0, 64), (2, 4))),
        "w_up": bell_draw(key_list[7], (EXPERTS, D, FF), D ** -0.5, 0.125, ((0, 64), (2, 4))),
        "w_down": bell_draw(key_list[8], (EXPERTS, FF, D), FF ** -0.5, 0.1875, ((0, 64), (2, 4))),
    }


def reference(tokens, group_choice, expert_choice, group_weight, expert_weight, norm_gain, w_gate, w_up, w_down):
    values = tokens.astype(jnp.float32)
    inv_rms = lax.rsqrt(lax.optimization_barrier(jnp.mean(values * values, -1, keepdims=True)) + 1e-06)
    normed = (values * inv_rms * norm_gain.astype(jnp.float32)).astype(jnp.bfloat16)
    expert_ids = (group_choice[:, None] * EXPERTS_GROUP + expert_choice).astype(jnp.int32)
    mixing = group_weight[:, None] * expert_weight / lax.optimization_barrier(jnp.sum(expert_weight, -1, keepdims=True))
    flat_ids = expert_ids.reshape(-1)
    flat_tokens = jnp.repeat(jnp.arange(TOKENS, dtype=jnp.int32), TOP_K)
    flat_mix = mixing.reshape(-1)
    ordering = jnp.argsort(flat_ids, stable=True).astype(jnp.int32)
    sorted_tokens = flat_tokens[ordering]
    sorted_mix = flat_mix[ordering]
    counts = lax.optimization_barrier(jnp.sum((flat_ids[None, :] == jnp.arange(EXPERTS, dtype=jnp.int32)[:, None]).astype(jnp.int32), 1))
    starts = jnp.cumsum(counts) - counts
    rows_most = TOKENS // TOK_DEV * CAP
    offsets = jnp.arange(rows_most, dtype=jnp.int32)

    def per_expert(summed, expert):
        places = jnp.minimum(starts[expert] + offsets, TOKENS * TOP_K - 1).astype(jnp.int32)
        alive = offsets < counts[expert]
        token_rows = sorted_tokens[places]
        weights = jnp.where(alive, sorted_mix[places], 0.0)
        chosen = normed[token_rows]
        gate_sum = jnp.dot(chosen, w_gate[expert], preferred_element_type=jnp.float32)
        up_sum = jnp.dot(chosen, w_up[expert], preferred_element_type=jnp.float32)
        hidden = (jax.nn.silu(gate_sum) * up_sum).astype(jnp.bfloat16)
        result = jnp.dot(hidden, w_down[expert], preferred_element_type=jnp.float32).astype(jnp.bfloat16)
        summed = summed.at[token_rows].add(result.astype(jnp.float32) * weights[:, None])
        return (summed, None)
    initial = jnp.zeros((TOKENS, D), jnp.float32)
    summed, _ = lax.scan(per_expert, initial, jnp.arange(EXPERTS, dtype=jnp.int32))
    return summed.astype(jnp.bfloat16)
```

```python
import jax
import jax.numpy as jnp
from jax import lax
from jax.sharding import Mesh
from jax.sharding import PartitionSpec as P

GRP_EP = ("grp", "g", "e")
EP = ("g", "e")
GROUP_SIZE = 8


def rank_before(marks):
    return jnp.cumsum(marks, -2) - marks


def body(
    tokens,
    group_choice,
    expert_choice,
    group_weight,
    expert_weight,
    norm_gain,
    w_gate,
    w_up,
    w_down,
):
    rows, width = tokens.shape
    groups = lax.axis_size("g")
    members = lax.axis_size("e")
    per_group = rows // groups
    mean_load = 2 * per_group // members
    capacity = mean_load + min(mean_load // 2, per_group - mean_load)
    model_width = norm_gain.shape[0]
    mixing = group_weight[:, None] * expert_weight / jnp.sum(expert_weight, -1, keepdims=True)

    group_marks = (group_choice[:, None] == jnp.arange(groups, dtype=jnp.int32)).astype(jnp.int32)
    place = group_choice * per_group + jnp.sum(rank_before(group_marks) * group_marks, 1)
    spots = jnp.arange(rows, dtype=jnp.int32)
    sort = spots[:, None] == place[None, :]

    values = tokens.astype(jnp.float32)
    squares = lax.all_gather(jnp.sum(values * values, -1), "tp", axis=0)
    inv_rms = lax.rsqrt(jnp.sum(squares, 0) / model_width + 1e-06)
    gain = lax.dynamic_slice_in_dim(norm_gain, lax.axis_index("tp") * width, width, 0)
    normed = (values * inv_rms[:, None] * gain[None, :]).astype(jnp.bfloat16)
    by_group = jnp.dot(
        sort.astype(jnp.bfloat16), normed, preferred_element_type=jnp.float32
    ).astype(jnp.bfloat16)
    facts = jnp.concatenate([expert_choice.astype(jnp.float32), mixing], -1)
    facts = jnp.dot(sort.astype(jnp.float32), facts, precision=lax.Precision.HIGHEST)
    landed = lax.all_to_all(
        by_group.reshape(groups, per_group, width), "g", 0, 0, tiled=True
    ).reshape(rows, width)
    facts = lax.all_to_all(
        facts.reshape(groups, per_group, 4), "g", 0, 0, tiled=True
    ).reshape(rows, 4)

    chosen = facts[:, :2].astype(jnp.int32).reshape(groups, per_group, 2)
    blocks = jnp.arange(groups, dtype=jnp.int32)[:, None, None]
    kinds = jnp.arange(members, dtype=jnp.int32)
    marks = jnp.sum((chosen[..., None] == kinds).astype(jnp.int32), 2)
    ranks = rank_before(marks)
    seats = jnp.sum(
        jnp.where(chosen[..., None] == kinds, ranks[:, :, None, :], 0), -1
    )
    targets = (chosen * groups + blocks) * capacity + seats
    targets = targets.reshape(rows, 2)
    seats_all = members * groups * capacity
    places = jnp.arange(seats_all, dtype=jnp.int32)
    picks = [targets[None, :, k] == places[:, None] for k in range(2)]
    dispatch = (picks[0] | picks[1]).astype(jnp.bfloat16)
    buffer = jnp.dot(dispatch, landed, preferred_element_type=jnp.float32).astype(jnp.bfloat16)
    received = lax.all_to_all(
        buffer.reshape(members, groups * capacity, width), "e", 0, 0, tiled=True
    ).reshape(seats_all, width)

    piece = lax.all_gather(received, "tp", axis=1, tiled=True)
    gate = jnp.dot(piece, w_gate[0], preferred_element_type=jnp.float32)
    up = jnp.dot(piece, w_up[0], preferred_element_type=jnp.float32)
    hidden = (jax.nn.silu(gate) * up).astype(jnp.bfloat16)
    hidden = lax.all_gather(hidden, "tp", axis=1, tiled=True)
    result = jnp.dot(hidden, w_down[0], preferred_element_type=jnp.float32).astype(jnp.bfloat16)
    back = lax.all_to_all(
        result.reshape(members, groups * capacity, width), "e", 0, 0, tiled=True
    ).reshape(seats_all, width)

    mixed = jnp.zeros((rows, width), jnp.float32)
    for k in range(2):
        picker = (targets[:, k : k + 1] == places[None, :]).astype(jnp.bfloat16)
        picked = jnp.dot(picker, back, preferred_element_type=jnp.float32)
        mixed = mixed + facts[:, 2 + k : 3 + k] * picked
    home = lax.all_to_all(
        mixed.astype(jnp.bfloat16).reshape(groups, per_group, width), "g", 0, 0, tiled=True
    ).reshape(rows, width)
    unsort = place[:, None] == spots[None, :]
    return jnp.dot(
        unsort.astype(jnp.bfloat16), home, preferred_element_type=jnp.float32
    ).astype(jnp.bfloat16)


def solution(mesh):
    members = GROUP_SIZE
    split = Mesh(
        mesh.devices.reshape(
            mesh.shape["grp"], mesh.shape["ep"] // members, members, mesh.shape["tp"]
        ),
        ("grp", "g", "e", "tp"),
    )
    placed = (
        P(GRP_EP, "tp"),
        P(GRP_EP),
        P(GRP_EP, None),
        P(GRP_EP),
        P(GRP_EP, None),
        P(),
        P(EP, None, "tp"),
        P(EP, None, "tp"),
        P(EP, None, "tp"),
    )
    return jax.shard_map(
        body, mesh=split, in_specs=placed, out_specs=P(GRP_EP, "tp"), check_vma=False
    )
```

```python
import functools

import jax
import jax.numpy as jnp
from jax import lax
from jax.experimental import pallas as pl
from jax.experimental.pallas import tpu as pltpu
from jax.sharding import Mesh
from jax.sharding import PartitionSpec as P

GRP_EP = ("grp", "g", "e")
EP = ("g", "e")
GROUP_SIZE = 8
MESH = pl.DeviceIdType.MESH
F32 = jnp.float32
BF16 = jnp.bfloat16


def dot(a, b):
    return jnp.dot(a, b, preferred_element_type=F32)


def iota(shape, dim):
    return lax.broadcasted_iota(jnp.int32, shape, dim)


def pieces(x, count):
    parts = []
    for _ in range(count):
        part = x.astype(BF16)
        parts.append(part)
        x = x - part.astype(F32)
    return parts


def remote(src, dst, send, recv, **where):
    return pltpu.make_async_remote_copy(
        src_ref=src, dst_ref=dst, send_sem=send, recv_sem=recv,
        device_id=where, device_id_type=MESH,
    )


def kernel(
    groups, members, ways, per_group, cap,
    tok, grow, gcol, crow, gw, ew, gain, wg_hbm, wu_hbm, wd_hbm,
    out,
    wg, wu, wd, sq, sorted_rows, facts, landed, facts_in, normed, rows_t, cols_t,
    picked, x, h, result, back, total, mixed, home,
    w_sem, q_send, q_recv, s1_send, s1_recv, m_send, m_recv, s2_send, s2_recv,
    x_send, x_recv, h_send, h_recv, r_send, r_recv, f_send, f_recv,
):
    my_g, my_e, my_t = lax.axis_index("g"), lax.axis_index("e"), lax.axis_index("tp")
    right, left = lax.rem(my_t + 1, ways), lax.rem(my_t + ways - 1, ways)
    across = lax.rem(my_t + 2, ways)
    rows, width = tok.shape
    chunk = groups * cap
    ff = wg.shape[1]
    lanes = 128

    loads = [
        pltpu.make_async_copy(src, dst, w_sem.at[n])
        for n, (src, dst) in enumerate(((wg_hbm, wg), (wu_hbm, wu), (wd_hbm, wd)))
    ]
    for load in loads:
        load.start()

    barrier = pltpu.get_barrier_semaphore()
    for off in range(1, groups):
        pl.semaphore_signal(
            barrier, inc=1, device_id={"g": lax.rem(my_g + off, groups)}, device_id_type=MESH
        )
    for off in range(1, members):
        pl.semaphore_signal(
            barrier, inc=1, device_id={"e": lax.rem(my_e + off, members)}, device_id_type=MESH
        )
    for off in range(1, ways):
        pl.semaphore_signal(
            barrier, inc=1, device_id={"tp": lax.rem(my_t + off, ways)}, device_id_type=MESH
        )

    earlier = iota((rows, rows), 0) < iota((rows, rows), 1)
    marks = (grow[...] == iota((groups, rows), 0)).astype(F32)
    rank_row = jnp.sum(dot(marks.astype(BF16), earlier.astype(BF16)) * marks, 0, keepdims=True)
    place_row = grow[...] * per_group + rank_row.astype(jnp.int32)
    sort = (iota((rows, rows), 0) == place_row).astype(BF16)
    sorted_rows[...] = dot(sort, tok[...]).astype(BF16).reshape(groups, per_group, width)
    values = tok[...].astype(F32)
    squares = jnp.sum(values * values, -1, keepdims=True)
    squares = jnp.transpose(jnp.broadcast_to(squares, (rows, lanes)))
    sq[my_t] = squares[:8]

    pl.semaphore_wait(barrier, groups + members + ways - 3)

    order = sorted(range(1, groups), key=lambda off: -min(off, groups - off))
    s1 = []
    q1 = []
    for off in range(1, ways):
        to = lax.rem(my_t + off, ways)
        q1.append(remote(sq.at[my_t], sq.at[my_t], q_send.at[to], q_recv.at[my_t], tp=to))
        q1[-1].start()
    for off in order:
        to = lax.rem(my_g + off, groups)
        s1.append(
            remote(sorted_rows.at[to], landed.at[my_g], s1_send.at[to], s1_recv.at[my_g], g=to)
        )
        s1[-1].start()
    landed[my_g] = sorted_rows[my_g]

    marks_c = (gcol[...] == iota((rows, groups), 1)).astype(F32)
    later = iota((rows, rows), 0) > iota((rows, rows), 1)
    rank_col = jnp.sum(dot(later.astype(BF16), marks_c.astype(BF16)) * marks_c, 1, keepdims=True)
    place_wide = gcol[...] * lanes + rank_col.astype(jnp.int32)
    spread = (iota((rows, groups * lanes), 1) == place_wide).astype(BF16)

    for off in range(1, ways):
        src = lax.rem(my_t + off, ways)
        remote(sq.at[src], sq.at[src], q_send.at[src], q_recv.at[src], tp=src).wait_recv()
    model_width = width * ways
    all_squares = jnp.sum(sq[...], 0)[:1]
    inv_rms = lax.rsqrt(all_squares / model_width + 1e-06)
    weights = ew[...]
    mixing = gw[...] * weights / jnp.sum(weights, 0, keepdims=True)
    choice = crow[...].astype(F32)
    fields = [choice[0:1], choice[1:2]]
    for k in range(2):
        fields += [p.astype(F32) for p in pieces(mixing[k : k + 1], 2)]
    fields += [p.astype(F32) for p in pieces(inv_rms, 3)]
    fields.append(jnp.zeros((16 - len(fields), rows), F32))
    fields = jnp.concatenate(fields, 0).astype(BF16)
    spread_fields = dot(fields, spread).astype(BF16)
    for n in range(groups):
        facts[n] = spread_fields[:, n * lanes : (n + 1) * lanes]
    m1 = []
    for off in order:
        to = lax.rem(my_g + off, groups)
        m1.append(remote(facts.at[to], facts_in.at[my_g], m_send.at[to], m_recv.at[my_g], g=to))
        m1[-1].start()
    facts_in[my_g] = facts[my_g]

    def block_of(shape, dim):
        spot = iota(shape, dim)
        block = jnp.zeros(shape, jnp.int32)
        for n in range(1, groups):
            block = block + (spot >= n * per_group).astype(jnp.int32)
        return block

    for off in order:
        src = lax.rem(my_g + off, groups)
        remote(facts.at[src], facts_in.at[src], m_send.at[src], m_recv.at[src], g=src).wait_recv()
    known = jnp.zeros((16, rows), F32)
    for n in range(groups):
        shift = (iota((lanes, rows), 0) + n * per_group == iota((lanes, rows), 1)).astype(BF16)
        known = known + dot(facts_in[n], shift)
    kinds = iota((members, rows), 0).astype(F32)
    on = [(known[k : k + 1] == kinds).astype(F32) for k in range(2)]
    same = block_of((rows, 1), 0) == block_of((1, rows), 1)
    before = (same & earlier).astype(BF16)
    ranks = dot((on[0] + on[1]).astype(BF16), before)
    base = (block_of((1, rows), 1) * cap).astype(F32)
    seats = [
        known[k : k + 1] * chunk + base + jnp.sum(on[k] * ranks, 0, keepdims=True)
        for k in range(2)
    ]
    inv = (known[6:7] + known[7:8]) + known[8:9]
    table = jnp.concatenate(
        [seats[0], seats[1], known[2:3], known[3:4], known[4:5], known[5:6], inv, inv], 0
    )
    rows_t[...] = table
    cols_t[...] = jnp.transpose(
        jnp.concatenate([table, jnp.zeros((lanes - 8, rows), F32)], 0)
    )

    for off in order:
        src = lax.rem(my_g + off, groups)
        remote(
            sorted_rows.at[src], landed.at[src], s1_send.at[src], s1_recv.at[src], g=src
        ).wait_recv()
    normed[...] = (
        landed[...].reshape(rows, width).astype(F32) * cols_t[:, 6:7] * gain[...]
    ).astype(BF16)

    def pick(member):
        spots = (iota((chunk, rows), 0) + member * chunk).astype(F32)
        chosen = (spots == rows_t[0:1]) | (spots == rows_t[1:2])
        return dot(chosen.astype(F32).astype(BF16), normed[...]).astype(BF16)

    x[my_t, my_e] = pick(my_e)

    def send_rows(step, carry):
        to = lax.rem(my_e + members - step, members)
        picked[to] = pick(to)
        remote(
            picked.at[to], x.at[my_t, my_e], s2_send.at[to], s2_recv.at[my_e], e=to
        ).start()
        return carry

    lax.fori_loop(1, members, send_rows, 0)
    total[...] = jnp.zeros_like(total)
    for load in loads:
        load.wait()

    def half(ref, src, e, n):
        part = ref.shape[3] // 2
        return ref.at[src, e, :, pl.ds(n * part, part)]

    def own_to(ref, send, recv, e, n):
        return remote(
            ref.at[my_t, e], ref.at[my_t, e], send.at[n, e], recv.at[n, e],
            tp=right if n == 0 else left,
        )

    def arrived(ref, send, recv, e, n):
        src = left if n == 0 else right
        return remote(
            ref.at[src, e], ref.at[src, e], send.at[n, e], recv.at[n, e],
            tp=right if n == 0 else left,
        )

    def pass_on(ref, send, recv, e, n):
        src = left if n == 0 else right
        return remote(
            half(ref, src, e, n), half(ref, src, e, n), send.at[2 + n, e], recv.at[2 + n, e],
            tp=right if n == 0 else left,
        )

    def passed(ref, send, recv, e, n):
        return remote(
            half(ref, across, e, n), half(ref, across, e, n), send.at[2 + n, e],
            recv.at[2 + n, e], tp=right if n == 0 else left,
        )

    def stage(step, lag, body):
        @pl.when((step >= lag) & (step < members + lag))
        def _():
            body(step - lag)

    def steps(step, carry):
        def enter(i):
            e = lax.rem(my_e + i, members)

            @pl.when(i > 0)
            def _():
                remote(
                    x.at[my_t, e], x.at[my_t, e], s2_send.at[e], s2_recv.at[e], e=e
                ).wait_recv()

            for n in range(2):
                own_to(x, x_send, x_recv, e, n).start()

        def forward_x(i):
            e = lax.rem(my_e + i, members)
            for n in range(2):
                arrived(x, x_send, x_recv, e, n).wait_recv()
                pass_on(x, x_send, x_recv, e, n).start()

        def widen(i):
            e = lax.rem(my_e + i, members)
            for n in range(2):
                passed(x, x_send, x_recv, e, n).wait_recv()
            gate = jnp.zeros((chunk, ff), F32)
            up = jnp.zeros((chunk, ff), F32)
            for t in range(ways):
                piece = x[t, e]
                gate = gate + dot(piece, wg[t * width : (t + 1) * width])
                up = up + dot(piece, wu[t * width : (t + 1) * width])
            h[my_t, e] = (gate / (1.0 + jnp.exp(-gate)) * up).astype(BF16)
            for n in range(2):
                own_to(h, h_send, h_recv, e, n).start()

        def forward_h(i):
            e = lax.rem(my_e + i, members)
            for n in range(2):
                arrived(h, h_send, h_recv, e, n).wait_recv()
                pass_on(h, h_send, h_recv, e, n).start()

        def narrow(i):
            e = lax.rem(my_e + i, members)
            for n in range(2):
                passed(h, h_send, h_recv, e, n).wait_recv()
            made = jnp.zeros((chunk, width), F32)
            for t in range(ways):
                made = made + dot(h[t, e], wd[t * ff : (t + 1) * ff])

            @pl.when(i == 0)
            def _():
                back[my_e] = made.astype(BF16)

            @pl.when(i > 0)
            def _():
                result[e] = made.astype(BF16)
                remote(
                    result.at[e], back.at[my_e], r_send.at[e], r_recv.at[my_e], e=e
                ).start()

        def mix(i):
            j = lax.rem(my_e + members - i, members)

            @pl.when(i > 0)
            def _():
                remote(
                    result.at[j], back.at[j], r_send.at[j], r_recv.at[j], e=j
                ).wait_recv()

            spots = (iota((rows, chunk), 1) + j * chunk).astype(F32)
            hit = [spots == cols_t[:, k : k + 1] for k in range(2)]
            part = jnp.zeros((rows, width), F32)
            for n in range(2):
                share = jnp.where(
                    hit[0], cols_t[:, 2 + n : 3 + n], jnp.where(hit[1], cols_t[:, 4 + n : 5 + n], 0.0)
                )
                part = part + dot(share.astype(BF16), back[j])
            total[...] += part

        stage(step, 0, enter)
        stage(step, 1, forward_x)
        stage(step, 3, forward_h)
        stage(step, 2, widen)
        stage(step, 4, narrow)
        stage(step, 6, mix)
        return carry

    lax.fori_loop(0, members + 6, steps, 0)

    mixed[...] = total[...].astype(BF16).reshape(groups, per_group, width)
    f1 = []
    for off in order:
        to = lax.rem(my_g + off, groups)
        f1.append(remote(mixed.at[to], home.at[my_g], f_send.at[to], f_recv.at[my_g], g=to))
        f1[-1].start()
    home[my_g] = mixed[my_g]
    place_col = gcol[...] * per_group + rank_col.astype(jnp.int32)
    unsort = (iota((rows, rows), 1) == place_col).astype(BF16)

    for copy in q1 + s1 + m1:
        copy.wait_send()

    def drain(step, carry):
        e = lax.rem(my_e + members - step, members)
        remote(
            picked.at[e], x.at[my_t, my_e], s2_send.at[e], s2_recv.at[my_e], e=e
        ).wait_send()
        remote(
            result.at[e], back.at[my_e], r_send.at[e], r_recv.at[my_e], e=e
        ).wait_send()
        return carry

    lax.fori_loop(1, members, drain, 0)

    def drain_ways(e, carry):
        for n in range(2):
            own_to(x, x_send, x_recv, e, n).wait_send()
            pass_on(x, x_send, x_recv, e, n).wait_send()
            own_to(h, h_send, h_recv, e, n).wait_send()
            pass_on(h, h_send, h_recv, e, n).wait_send()
        return carry

    lax.fori_loop(0, members, drain_ways, 0)

    for off in order:
        src = lax.rem(my_g + off, groups)
        remote(mixed.at[src], home.at[src], f_send.at[src], f_recv.at[src], g=src).wait_recv()
    for copy in f1:
        copy.wait_send()
    out[...] = dot(unsort, home[...].reshape(rows, width)).astype(BF16)


def body(
    tokens,
    group_choice,
    expert_choice,
    group_weight,
    expert_weight,
    norm_gain,
    w_gate,
    w_up,
    w_down,
):
    rows, width = tokens.shape
    groups, members, ways = lax.axis_size("g"), lax.axis_size("e"), lax.axis_size("tp")
    per_group = rows // groups
    mean_load = 2 * per_group // members
    cap = mean_load + min(mean_load // 2, per_group - mean_load)
    chunk = groups * cap
    ff = w_gate.shape[2]
    gain = lax.dynamic_slice_in_dim(norm_gain, lax.axis_index("tp") * width, width, 0)
    dma = pltpu.SemaphoreType.DMA
    vmem = pl.BlockSpec(memory_space=pltpu.VMEM)
    hbm = pl.BlockSpec(memory_space=pl.ANY)
    return pl.pallas_call(
        functools.partial(kernel, groups, members, ways, per_group, cap),
        out_shape=jax.ShapeDtypeStruct((rows, width), BF16),
        in_specs=[vmem] * 7 + [hbm] * 3,
        out_specs=vmem,
        scratch_shapes=[
            pltpu.VMEM((ways * width, ff), BF16),
            pltpu.VMEM((ways * width, ff), BF16),
            pltpu.VMEM((ways * ff, width), BF16),
            pltpu.VMEM((ways, 8, rows), F32),
            pltpu.VMEM((groups, per_group, width), BF16),
            pltpu.VMEM((groups, 16, 128), BF16),
            pltpu.VMEM((groups, per_group, width), BF16),
            pltpu.VMEM((groups, 16, 128), BF16),
            pltpu.VMEM((rows, width), BF16),
            pltpu.VMEM((8, rows), F32),
            pltpu.VMEM((rows, 128), F32),
            pltpu.VMEM((members, chunk, width), BF16),
            pltpu.VMEM((ways, members, chunk, width), BF16),
            pltpu.VMEM((ways, members, chunk, ff), BF16),
            pltpu.VMEM((members, chunk, width), BF16),
            pltpu.VMEM((members, chunk, width), BF16),
            pltpu.VMEM((rows, width), F32),
            pltpu.VMEM((groups, per_group, width), BF16),
            pltpu.VMEM((groups, per_group, width), BF16),
            dma((3,)),
            dma((ways,)), dma((ways,)),
            dma((groups,)), dma((groups,)),
            dma((groups,)), dma((groups,)),
            dma((members,)), dma((members,)),
            dma((4, members)), dma((4, members)),
            dma((4, members)), dma((4, members)),
            dma((members,)), dma((members,)),
            dma((groups,)), dma((groups,)),
        ],
        compiler_params=pltpu.CompilerParams(
            collective_id=0, has_side_effects=True, vmem_limit_bytes=48 * 1024 * 1024
        ),
        name="expert_layer",
    )(
        tokens,
        group_choice[None, :],
        group_choice[:, None],
        expert_choice.T,
        group_weight[None, :],
        expert_weight.T,
        gain[None, :],
        w_gate[0],
        w_up[0],
        w_down[0],
    )


def solution(mesh):
    members = GROUP_SIZE
    split = Mesh(
        mesh.devices.reshape(
            mesh.shape["grp"], mesh.shape["ep"] // members, members, mesh.shape["tp"]
        ),
        ("grp", "g", "e", "tp"),
    )
    placed = (
        P(GRP_EP, "tp"),
        P(GRP_EP),
        P(GRP_EP, None),
        P(GRP_EP),
        P(GRP_EP, None),
        P(),
        P(EP, None, "tp"),
        P(EP, None, "tp"),
        P(EP, None, "tp"),
    )
    return jax.shard_map(
        body, mesh=split, in_specs=placed, out_specs=P(GRP_EP, "tp"), check_vma=False
    )
```

```python
import functools

import jax
import jax.numpy as jnp
from jax import lax
from jax.experimental import pallas as pl
from jax.experimental.pallas import tpu as pltpu
from jax.sharding import Mesh
from jax.sharding import PartitionSpec as P

GRP_EP = ("grp", "g", "e")
EP = ("g", "e")
GROUP_SIZE = 8
MESH = pl.DeviceIdType.MESH
F32 = jnp.float32
BF16 = jnp.bfloat16


def dot(a, b):
    return jnp.dot(a, b, preferred_element_type=F32)


def iota(shape, dim):
    return lax.broadcasted_iota(jnp.int32, shape, dim)


def pieces(x, count):
    parts = []
    for _ in range(count):
        part = x.astype(BF16)
        parts.append(part)
        x = x - part.astype(F32)
    return parts


def remote(src, dst, send, recv, **where):
    return pltpu.make_async_remote_copy(
        src_ref=src, dst_ref=dst, send_sem=send, recv_sem=recv,
        device_id=where, device_id_type=MESH,
    )


LAGS = (0, 2, 4, 6, 8, 11)
LEAD_AT = 5
SENDS = ((1, 7, 2, 6), (3, 5, 4))
PHASES = 2


def kernel(
    groups, members, ways, per_group, cap,
    tok_hbm, grow, crow, gw, ew, gain, wg_hbm, wu_hbm, wd_hbm,
    out,
    tok, wg, wu, wd, sq, sorted_rows, facts, landed, facts_in, normed, rows_t, cols_t,
    picked, x, h, result, back, total, mixed, home,
    w_sem, q_send, q_recv, s1_send, s1_recv, m_send, m_recv, s2_send, s2_recv,
    x_send, x_recv, h_send, h_recv, r_send, r_recv, f_send, f_recv,
):
    my_g, my_e, my_t = lax.axis_index("g"), lax.axis_index("e"), lax.axis_index("tp")
    right, left = lax.rem(my_t + 1, ways), lax.rem(my_t + ways - 1, ways)
    across = lax.rem(my_t + 2, ways)
    rows, width = tok.shape
    slots = groups // PHASES
    some = rows // PHASES
    chunk = slots * cap
    chunks = PHASES * members
    ff = wg.shape[1]
    lanes = 128
    wide = 2 * lanes

    tok_load = pltpu.make_async_copy(tok_hbm, tok, w_sem.at[3])
    tok_load.start()
    loads = [
        pltpu.make_async_copy(src, dst, w_sem.at[n])
        for n, (src, dst) in enumerate(((wg_hbm, wg), (wu_hbm, wu), (wd_hbm, wd)))
    ]
    for load in loads:
        load.start()

    barrier = pltpu.get_barrier_semaphore()

    def greet(**where):
        pl.semaphore_signal(barrier, inc=1, device_id=where, device_id_type=MESH)

    near = members // 2
    my_part = my_e // near

    def leader_of(k):
        if k == near:
            return lax.rem(my_e + near, members)
        return (k // near) * near + lax.rem(my_e + k, near)

    def slot_there(k):
        if k == near:
            return groups - 2
        return 2 * (min(k, groups - k) - 1) + my_part

    def source_of(slot):
        if slot == groups - 2:
            return near, lax.rem(my_e + near, members)
        away = slot // 2 + 1
        k = away + my_part * (groups - 2 * away)
        return k, lax.rem(my_e + groups - k, near) + (slot % 2) * near

    def back_by(k):
        return lax.rem(my_g + groups - k, groups)

    for k in range(1, groups):
        greet(g=lax.rem(my_g + k, groups), e=leader_of(k))
    for slot in range(groups - 1):
        k, e = source_of(slot)
        greet(g=back_by(k), e=e)
    for off in range(1, members):
        greet(e=lax.rem(my_e + off, members))
    for off in range(1, ways):
        greet(tp=lax.rem(my_t + off, ways))

    earlier = iota((rows, rows), 0) < iota((rows, rows), 1)
    marks = (grow[...] == iota((groups, rows), 0)).astype(F32)
    rank_row = jnp.sum(dot(marks.astype(BF16), earlier.astype(BF16)) * marks, 0, keepdims=True)
    place_row = grow[...] * per_group + rank_row.astype(jnp.int32)
    sort = (iota((rows, rows), 0) == place_row).astype(BF16)
    two = jnp.concatenate(
        [place_row.astype(F32), grow[...] * lanes + rank_row, jnp.zeros((lanes - 2, rows), F32)], 0
    )
    place_cols = jnp.transpose(two)
    place_col, place_wide = place_cols[:, 0:1], place_cols[:, 1:2]
    tok_load.wait()
    sorted_rows[...] = dot(sort, tok[...]).astype(BF16).reshape(groups, per_group, width)
    values = tok[...].astype(F32)
    squares = jnp.sum(values * values, -1, keepdims=True)
    squares = jnp.transpose(jnp.broadcast_to(squares, (rows, lanes)))
    sq[my_t] = squares[:8]

    with jax.named_scope("barrier_wait"):
        pl.semaphore_wait(barrier, 2 * groups + members + ways - 4)

    def rows_out(k):
        to = lax.rem(my_g + k, groups)
        slot = slot_there(k)
        return remote(
            sorted_rows.at[to], landed.at[slot], s1_send.at[k], s1_recv.at[slot],
            g=to, e=leader_of(k),
        )

    def rows_in(slot):
        k, e = source_of(slot)
        return remote(
            sorted_rows.at[slot], landed.at[slot], s1_send.at[slot], s1_recv.at[slot],
            g=back_by(k), e=e,
        )

    def facts_out(k):
        to = lax.rem(my_g + k, groups)
        slot = slot_there(k)
        return remote(
            facts.at[to], facts_in.at[slot], m_send.at[k], m_recv.at[slot],
            g=to, e=leader_of(k),
        )

    def facts_to_me(slot):
        k, e = source_of(slot)
        return remote(
            facts.at[slot], facts_in.at[slot], m_send.at[slot], m_recv.at[slot],
            g=back_by(k), e=e,
        )

    def home_out(slot):
        k, e = source_of(slot)
        return remote(
            mixed.at[slot], home.at[my_g], f_send.at[slot], f_recv.at[k], g=back_by(k), e=e
        )

    def home_in(k):
        src = lax.rem(my_g + k, groups)
        return remote(
            mixed.at[k], home.at[src], f_send.at[k], f_recv.at[k], g=src, e=leader_of(k)
        )

    q1 = []
    for off in range(1, ways):
        to = lax.rem(my_t + off, ways)
        q1.append(remote(sq.at[my_t], sq.at[my_t], q_send.at[to], q_recv.at[my_t], tp=to))
        q1[-1].start()
    for k in SENDS[0]:
        rows_out(k).start()
    landed[groups - 1] = sorted_rows[my_g]

    spread = (iota((rows, groups * lanes), 1).astype(F32) == place_wide).astype(BF16)
    with jax.named_scope("sq_wait"):
        for off in range(1, ways):
            src = lax.rem(my_t + off, ways)
            remote(sq.at[src], sq.at[src], q_send.at[src], q_recv.at[src], tp=src).wait_recv()
    model_width = width * ways
    all_squares = jnp.sum(sq[...], 0)[:1]
    inv_rms = lax.rsqrt(all_squares / model_width + 1e-06)
    weights = ew[...]
    mixing = gw[...] * weights / jnp.sum(weights, 0, keepdims=True)
    choice = crow[...].astype(F32)
    fields = [choice[0:1], choice[1:2]]
    for k in range(2):
        fields += [p.astype(F32) for p in pieces(mixing[k : k + 1], 2)]
    fields += [p.astype(F32) for p in pieces(inv_rms, 3)]
    fields.append(jnp.zeros((16 - len(fields), rows), F32))
    fields = jnp.concatenate(fields, 0).astype(BF16)
    spread_fields = dot(fields, spread).astype(BF16)
    for n in range(groups):
        facts[n] = spread_fields[:, n * lanes : (n + 1) * lanes]
    for k in SENDS[0] + SENDS[1]:
        facts_out(k).start()
    facts_in[groups - 1] = facts[my_g]
    for load in loads:
        load.wait()

    def block_of(shape, dim):
        spot = iota(shape, dim)
        block = jnp.zeros(shape, jnp.int32)
        for n in range(1, slots):
            block = block + (spot >= n * per_group).astype(jnp.int32)
        return block

    def lead(phase):
        first = phase * slots
        with jax.named_scope("facts_wait"):
            for slot in range(first, min(first + slots, groups - 1)):
                facts_to_me(slot).wait_recv()
        known = jnp.zeros((16, wide), F32)
        for n in range(slots):
            shift = (iota((lanes, wide), 0) + n * per_group == iota((lanes, wide), 1)).astype(BF16)
            known = known + dot(facts_in[first + n], shift)
        kinds = iota((members, wide), 0).astype(F32)
        on = [(known[k : k + 1] == kinds).astype(F32) for k in range(2)]
        same = block_of((wide, 1), 0) == block_of((1, wide), 1)
        before = (same & (iota((wide, wide), 0) < iota((wide, wide), 1))).astype(BF16)
        ranks = dot((on[0] + on[1]).astype(BF16), before)
        base = (block_of((1, wide), 1) * cap).astype(F32)
        seats = [
            known[k : k + 1] * chunk + base + jnp.sum(on[k] * ranks, 0, keepdims=True)
            for k in range(2)
        ]
        inv = (known[6:7] + known[7:8]) + known[8:9]
        table = jnp.concatenate(
            [seats[0], seats[1], known[2:3], known[3:4], known[4:5], known[5:6], inv, inv], 0
        )
        rows_t[phase] = table
        cols_t[phase] = jnp.transpose(
            jnp.concatenate([table, jnp.zeros((lanes - 8, wide), F32)], 0)
        )
        with jax.named_scope("landed_wait"):
            for slot in range(first, min(first + slots, groups - 1)):
                rows_in(slot).wait_recv()
        if phase == 0:
            for k in SENDS[1]:
                rows_out(k).start()
        scale = gain[:, pl.ds(pl.multiple_of(my_t * width, width), width)]
        normed[...] = (
            landed[first : first + slots].reshape(some, width).astype(F32)
            * cols_t[phase, :some, 6:7]
            * scale
        ).astype(BF16)

        def pick(member):
            spots = (iota((chunk, some), 0) + member * chunk).astype(F32)
            chosen = (spots == rows_t[phase, 0:1, :some]) | (spots == rows_t[phase, 1:2, :some])
            return dot(chosen.astype(F32).astype(BF16), normed[...]).astype(BF16)

        x[my_t, phase * members + my_e] = pick(my_e)

        def send_rows(step, carry):
            to = lax.rem(my_e + members - step, members)
            picked[phase * members + to] = pick(to)
            rows_to(phase * members + to, phase * members + my_e, to).start()
            return carry

        lax.fori_loop(1, members, send_rows, 0)

    def rows_to(there, here, to):
        return remote(
            picked.at[there], x.at[my_t, here], s2_send.at[there], s2_recv.at[here], e=to
        )

    def result_to(there, here, to):
        return remote(
            result.at[there], back.at[here], r_send.at[there], r_recv.at[here], e=to
        )

    def half(ref, src, c, n):
        part = ref.shape[3] // 2
        return ref.at[src, c, :, pl.ds(n * part, part)]

    def own_to(ref, send, recv, c, n):
        return remote(
            ref.at[my_t, c], ref.at[my_t, c], send.at[n, c], recv.at[n, c],
            tp=right if n == 0 else left,
        )

    def arrived(ref, send, recv, c, n):
        src = left if n == 0 else right
        return remote(
            ref.at[src, c], ref.at[src, c], send.at[n, c], recv.at[n, c],
            tp=right if n == 0 else left,
        )

    def pass_on(ref, send, recv, c, n):
        src = left if n == 0 else right
        return remote(
            half(ref, src, c, n), half(ref, src, c, n), send.at[2 + n, c], recv.at[2 + n, c],
            tp=right if n == 0 else left,
        )

    def passed(ref, send, recv, c, n):
        return remote(
            half(ref, across, c, n), half(ref, across, c, n), send.at[2 + n, c],
            recv.at[2 + n, c], tp=right if n == 0 else left,
        )

    def enter(i, off, phase, e, c):
        @pl.when(off > 0)
        def _():
            rows_to(c, c, e).wait_recv()

        for n in range(2):
            own_to(x, x_send, x_recv, c, n).start()

    def forward_x(i, off, phase, e, c):
        for n in range(2):
            arrived(x, x_send, x_recv, c, n).wait_recv()
            pass_on(x, x_send, x_recv, c, n).start()

    def widen(i, off, phase, e, c):
        for n in range(2):
            passed(x, x_send, x_recv, c, n).wait_recv()
        gate = jnp.zeros((chunk, ff), F32)
        up = jnp.zeros((chunk, ff), F32)
        for t in range(ways):
            piece = x[t, c]
            gate = gate + dot(piece, wg[t * width : (t + 1) * width])
            up = up + dot(piece, wu[t * width : (t + 1) * width])
        h[my_t, c] = (gate / (1.0 + jnp.exp(-gate)) * up).astype(BF16)
        for n in range(2):
            own_to(h, h_send, h_recv, c, n).start()

    def forward_h(i, off, phase, e, c):
        for n in range(2):
            arrived(h, h_send, h_recv, c, n).wait_recv()
            pass_on(h, h_send, h_recv, c, n).start()

    def narrow(i, off, phase, e, c):
        for n in range(2):
            passed(h, h_send, h_recv, c, n).wait_recv()
        made = jnp.zeros((chunk, width), F32)
        for t in range(ways):
            made = made + dot(h[t, c], wd[t * ff : (t + 1) * ff])

        @pl.when(off == 0)
        def _():
            back[c] = made.astype(BF16)

        @pl.when(off > 0)
        def _():
            result[c] = made.astype(BF16)
            result_to(c, phase * members + my_e, e).start()

    def mix(i, off, phase, e, c):
        j = lax.rem(my_e + members - off, members)
        there = phase * members + j

        @pl.when(off > 0)
        def _():
            result_to(there, there, j).wait_recv()

        spots = (iota((some, chunk), 1) + j * chunk).astype(F32)
        hit = [spots == cols_t[phase, :some, k : k + 1] for k in range(2)]
        part = jnp.zeros((some, width), F32)
        for n in range(2):
            share = jnp.where(
                hit[0],
                cols_t[phase, :some, 2 + n : 3 + n],
                jnp.where(hit[1], cols_t[phase, :some, 4 + n : 5 + n], 0.0),
            )
            part = part + dot(share.astype(BF16), back[there])

        @pl.when(off == 0)
        def _():
            total[...] = part

        @pl.when(off > 0)
        def _():
            total[...] += part

        for p in range(PHASES):
            @pl.when(i == (p + 1) * members - 1)
            def _():
                first = p * slots
                mixed[first : first + slots] = (
                    total[...].astype(BF16).reshape(slots, per_group, width)
                )
                for slot in range(first, min(first + slots, groups - 1)):
                    home_out(slot).start()

    def stage(step, lag, name, body):
        with jax.named_scope(name):
            @pl.when((step >= lag) & (step < chunks + lag))
            def _():
                i = step - lag
                phase, off = i // members, lax.rem(i, members)
                e = lax.rem(my_e + off, members)
                body(i, off, phase, e, phase * members + e)

    def steps(step, carry):
        stage(step, LAGS[0], "enter", enter)
        stage(step, LAGS[1], "forward_x", forward_x)
        stage(step, LAGS[3], "forward_h", forward_h)
        stage(step, LAGS[2], "widen", widen)
        stage(step, LAGS[4], "narrow", narrow)
        stage(step, LAGS[5], "mix", mix)

        @pl.when(step == LEAD_AT)
        def _():
            lead(1)

        return carry

    lead(0)
    lax.fori_loop(0, chunks + LAGS[5], steps, 0)
    home[my_g] = mixed[groups - 1]
    unsort = (iota((rows, rows), 1).astype(F32) == place_col).astype(BF16)

    for copy in q1:
        copy.wait_send()
    for k in range(1, groups):
        rows_out(k).wait_send()
        facts_out(k).wait_send()

    def drain(step, carry):
        phase, off = step // members, lax.rem(step, members)

        @pl.when(off > 0)
        def _():
            e = lax.rem(my_e + off, members)
            rows_to(phase * members + e, phase * members + my_e, e).wait_send()
            result_to(phase * members + e, phase * members + my_e, e).wait_send()

        for n in range(2):
            own_to(x, x_send, x_recv, step, n).wait_send()
            pass_on(x, x_send, x_recv, step, n).wait_send()
            own_to(h, h_send, h_recv, step, n).wait_send()
            pass_on(h, h_send, h_recv, step, n).wait_send()
        return carry

    lax.fori_loop(0, chunks, drain, 0)
    with jax.named_scope("home_wait"):
        for k in range(1, groups):
            home_in(k).wait_recv()
    for slot in range(groups - 1):
        home_out(slot).wait_send()
    out[...] = dot(unsort, home[...].reshape(rows, width)).astype(BF16)


def body(
    tokens,
    group_choice,
    expert_choice,
    group_weight,
    expert_weight,
    norm_gain,
    w_gate,
    w_up,
    w_down,
):
    rows, width = tokens.shape
    groups, members, ways = lax.axis_size("g"), lax.axis_size("e"), lax.axis_size("tp")
    per_group = rows // groups
    mean_load = 2 * per_group // members
    cap = mean_load + min(mean_load // 2, per_group - mean_load)
    chunk = groups // PHASES * cap
    chunks = PHASES * members
    some = rows // PHASES
    ff = w_gate.shape[2]
    dma = pltpu.SemaphoreType.DMA
    vmem = pl.BlockSpec(memory_space=pltpu.VMEM)
    hbm = pl.BlockSpec(memory_space=pltpu.HBM)
    return pl.pallas_call(
        functools.partial(kernel, groups, members, ways, per_group, cap),
        out_shape=jax.ShapeDtypeStruct((rows, width), BF16),
        in_specs=[hbm] + [vmem] * 5 + [hbm] * 3,
        out_specs=vmem,
        scratch_shapes=[
            pltpu.VMEM((rows, width), BF16),
            pltpu.VMEM((ways * width, ff), BF16),
            pltpu.VMEM((ways * width, ff), BF16),
            pltpu.VMEM((ways * ff, width), BF16),
            pltpu.VMEM((ways, 8, rows), F32),
            pltpu.VMEM((groups, per_group, width), BF16),
            pltpu.VMEM((groups, 16, 128), BF16),
            pltpu.VMEM((groups, per_group, width), BF16),
            pltpu.VMEM((groups, 16, 128), BF16),
            pltpu.VMEM((some, width), BF16),
            pltpu.VMEM((PHASES, 8, 256), F32),
            pltpu.VMEM((PHASES, 256, 128), F32),
            pltpu.VMEM((chunks, chunk, width), BF16),
            pltpu.VMEM((ways, chunks, chunk, width), BF16),
            pltpu.VMEM((ways, chunks, chunk, ff), BF16),
            pltpu.VMEM((chunks, chunk, width), BF16),
            pltpu.VMEM((chunks, chunk, width), BF16),
            pltpu.VMEM((some, width), F32),
            pltpu.VMEM((groups, per_group, width), BF16),
            pltpu.VMEM((groups, per_group, width), BF16),
            dma((4,)),
            dma((ways,)), dma((ways,)),
            dma((groups,)), dma((groups,)),
            dma((groups,)), dma((groups,)),
            dma((chunks,)), dma((chunks,)),
            dma((4, chunks)), dma((4, chunks)),
            dma((4, chunks)), dma((4, chunks)),
            dma((chunks,)), dma((chunks,)),
            dma((groups,)), dma((groups,)),
        ],
        compiler_params=pltpu.CompilerParams(
            collective_id=0, has_side_effects=True, vmem_limit_bytes=62 * 1024 * 1024
        ),
        name="expert_layer",
    )(
        tokens,
        group_choice[None, :],
        expert_choice.T,
        group_weight[None, :],
        expert_weight.T,
        norm_gain[None, :],
        w_gate[0],
        w_up[0],
        w_down[0],
    )


def solution(mesh):
    members = GROUP_SIZE
    split = Mesh(
        mesh.devices.reshape(
            mesh.shape["grp"], mesh.shape["ep"] // members, members, mesh.shape["tp"]
        ),
        ("grp", "g", "e", "tp"),
    )
    placed = (
        P(GRP_EP, "tp"),
        P(GRP_EP),
        P(GRP_EP, None),
        P(GRP_EP),
        P(GRP_EP, None),
        P(),
        P(EP, None, "tp"),
        P(EP, None, "tp"),
        P(EP, None, "tp"),
    )
    return jax.shard_map(
        body, mesh=split, in_specs=placed, out_specs=P(GRP_EP, "tp"), check_vma=False
    )
```

```python
import functools

import jax
import jax.numpy as jnp
from jax import lax
from jax.experimental import pallas as pl
from jax.experimental.pallas import tpu as pltpu
from jax.sharding import Mesh
from jax.sharding import PartitionSpec as P

GRP_EP = ("grp", "g", "e")
EP = ("g", "e")
GROUP_SIZE = 8
MESH = pl.DeviceIdType.MESH
F32 = jnp.float32
BF16 = jnp.bfloat16


def dot(a, b):
    return jnp.dot(a, b, preferred_element_type=F32)


def iota(shape, dim):
    return lax.broadcasted_iota(jnp.int32, shape, dim)


def pieces(x, count):
    parts = []
    for _ in range(count):
        part = x.astype(BF16)
        parts.append(part)
        x = x - part.astype(F32)
    return parts


def remote(src, dst, send, recv, **where):
    return pltpu.make_async_remote_copy(
        src_ref=src, dst_ref=dst, send_sem=send, recv_sem=recv,
        device_id=where, device_id_type=MESH,
    )


LAGS = (0, 2, 4, 7, 9, 13)
AWAY = (1, 4, 3, 2)
PHASES = 4
LEAD_AT = (6, 14, 22)
UPFRONT = 2


def kernel(
    groups, members, ways, per_group, cap,
    tok_hbm, grow, crow, gw, ew, gain, wg_hbm, wu_hbm, wd_hbm,
    out,
    tok, wg, wu, wd, sq, sorted_rows, facts, landed, facts_in, normed, rows_t, cols_t,
    picked, x, h, result, back, total, mixed, home,
    w_sem, q_send, q_recv, s1_send, s1_recv, m_send, m_recv, s2_send, s2_recv,
    x_send, x_recv, h_send, h_recv, r_send, r_recv, f_send, f_recv,
):
    my_g, my_e, my_t = lax.axis_index("g"), lax.axis_index("e"), lax.axis_index("tp")
    right, left = lax.rem(my_t + 1, ways), lax.rem(my_t + ways - 1, ways)
    across = lax.rem(my_t + 2, ways)
    rows, width = tok.shape
    slots = groups // PHASES
    some = rows // PHASES
    chunk = slots * cap
    chunks = PHASES * members
    ff = wg.shape[1]
    lanes = 128
    wide = -(-some // lanes) * lanes

    tok_load = pltpu.make_async_copy(tok_hbm, tok, w_sem.at[3])
    tok_load.start()
    loads = [
        pltpu.make_async_copy(src, dst, w_sem.at[n])
        for n, (src, dst) in enumerate(((wg_hbm, wg), (wu_hbm, wu), (wd_hbm, wd)))
    ]
    for load in loads:
        load.start()

    barrier = pltpu.get_barrier_semaphore()

    def greet(**where):
        pl.semaphore_signal(barrier, inc=1, device_id=where, device_id_type=MESH)

    near = members // 2
    home_slot = 2 * AWAY.index(near) + 1
    per_phase = len(AWAY) // PHASES
    sends = [
        sum([(a,) if a == near else (a, groups - a) for a in AWAY[n : n + per_phase]], ())
        for n in range(0, len(AWAY), per_phase)
    ]

    def slots_of(phase):
        every = range(groups // PHASES * phase, groups // PHASES * (phase + 1))
        return [slot for slot in every if slot != home_slot]

    my_part = my_e // near

    def leader_of(k):
        if k == near:
            return lax.rem(my_e + near, members)
        return (k // near) * near + lax.rem(my_e + k, near)

    def slot_there(k):
        if k == near:
            return home_slot - 1
        return 2 * AWAY.index(min(k, groups - k)) + my_part

    def source_of(slot):
        if slot == home_slot - 1:
            return near, lax.rem(my_e + near, members)
        away = AWAY[slot // 2]
        k = away + my_part * (groups - 2 * away)
        return k, lax.rem(my_e + groups - k, near) + (slot % 2) * near

    def back_by(k):
        return lax.rem(my_g + groups - k, groups)

    for k in range(1, groups):
        greet(g=lax.rem(my_g + k, groups), e=leader_of(k))
    for phase in range(PHASES):
        for slot in slots_of(phase):
            k, e = source_of(slot)
            greet(g=back_by(k), e=e)
    for off in range(1, members):
        greet(e=lax.rem(my_e + off, members))
    for off in range(1, ways):
        greet(tp=lax.rem(my_t + off, ways))

    earlier = iota((rows, rows), 0) < iota((rows, rows), 1)
    marks = (grow[...] == iota((groups, rows), 0)).astype(F32)
    rank_row = jnp.sum(dot(marks.astype(BF16), earlier.astype(BF16)) * marks, 0, keepdims=True)
    place_row = grow[...] * per_group + rank_row.astype(jnp.int32)
    sort = (iota((rows, rows), 0) == place_row).astype(BF16)
    two = jnp.concatenate(
        [place_row.astype(F32), grow[...] * lanes + rank_row, jnp.zeros((lanes - 2, rows), F32)], 0
    )
    place_cols = jnp.transpose(two)
    place_col, place_wide = place_cols[:, 0:1], place_cols[:, 1:2]
    tok_load.wait()
    sorted_rows[...] = dot(sort, tok[...]).astype(BF16).reshape(groups, per_group, width)
    values = tok[...].astype(F32)
    squares = jnp.sum(values * values, -1, keepdims=True)
    squares = jnp.transpose(jnp.broadcast_to(squares, (rows, lanes)))
    sq[my_t] = squares[:8]

    with jax.named_scope("barrier_wait"):
        pl.semaphore_wait(barrier, 2 * groups + members + ways - 4)

    def rows_out(k):
        to = lax.rem(my_g + k, groups)
        slot = slot_there(k)
        return remote(
            sorted_rows.at[to], landed.at[slot], s1_send.at[k], s1_recv.at[slot],
            g=to, e=leader_of(k),
        )

    def rows_in(slot):
        k, e = source_of(slot)
        return remote(
            sorted_rows.at[slot], landed.at[slot], s1_send.at[slot], s1_recv.at[slot],
            g=back_by(k), e=e,
        )

    def facts_out(k):
        to = lax.rem(my_g + k, groups)
        slot = slot_there(k)
        return remote(
            facts.at[to], facts_in.at[slot], m_send.at[k], m_recv.at[slot],
            g=to, e=leader_of(k),
        )

    def facts_to_me(slot):
        k, e = source_of(slot)
        return remote(
            facts.at[slot], facts_in.at[slot], m_send.at[slot], m_recv.at[slot],
            g=back_by(k), e=e,
        )

    def home_out(slot):
        k, e = source_of(slot)
        return remote(
            mixed.at[slot], home.at[my_g], f_send.at[slot], f_recv.at[k], g=back_by(k), e=e
        )

    def home_in(k):
        src = lax.rem(my_g + k, groups)
        return remote(
            mixed.at[k], home.at[src], f_send.at[k], f_recv.at[k], g=src, e=leader_of(k)
        )

    q1 = []
    for off in range(1, ways):
        to = lax.rem(my_t + off, ways)
        q1.append(remote(sq.at[my_t], sq.at[my_t], q_send.at[to], q_recv.at[my_t], tp=to))
        q1[-1].start()
    for k in sum(sends[:UPFRONT], ()):
        rows_out(k).start()
    landed[home_slot] = sorted_rows[my_g]

    spread = (iota((rows, groups * lanes), 1).astype(F32) == place_wide).astype(BF16)
    with jax.named_scope("sq_wait"):
        for off in range(1, ways):
            src = lax.rem(my_t + off, ways)
            remote(sq.at[src], sq.at[src], q_send.at[src], q_recv.at[src], tp=src).wait_recv()
    model_width = width * ways
    all_squares = jnp.sum(sq[...], 0)[:1]
    inv_rms = lax.rsqrt(all_squares / model_width + 1e-06)
    weights = ew[...]
    mixing = gw[...] * weights / jnp.sum(weights, 0, keepdims=True)
    choice = crow[...].astype(F32)
    fields = [choice[0:1], choice[1:2]]
    for k in range(2):
        fields += [p.astype(F32) for p in pieces(mixing[k : k + 1], 2)]
    fields += [p.astype(F32) for p in pieces(inv_rms, 3)]
    fields.append(jnp.zeros((16 - len(fields), rows), F32))
    fields = jnp.concatenate(fields, 0).astype(BF16)
    spread_fields = dot(fields, spread).astype(BF16)
    for n in range(groups):
        facts[n] = spread_fields[:, n * lanes : (n + 1) * lanes]
    for k in sum(sends, ()):
        facts_out(k).start()
    facts_in[home_slot] = facts[my_g]
    for load in loads:
        load.wait()

    def block_of(shape, dim):
        spot = iota(shape, dim)
        block = jnp.zeros(shape, jnp.int32)
        for n in range(1, slots):
            block = block + (spot >= n * per_group).astype(jnp.int32)
        return block

    def lead(phase):
        first = phase * slots
        with jax.named_scope("facts_wait"):
            for slot in slots_of(phase):
                facts_to_me(slot).wait_recv()
        known = jnp.zeros((16, wide), F32)
        for n in range(slots):
            shift = (iota((lanes, wide), 0) + n * per_group == iota((lanes, wide), 1)).astype(BF16)
            known = known + dot(facts_in[first + n], shift)
        kinds = iota((members, wide), 0).astype(F32)
        on = [(known[k : k + 1] == kinds).astype(F32) for k in range(2)]
        same = block_of((wide, 1), 0) == block_of((1, wide), 1)
        before = (same & (iota((wide, wide), 0) < iota((wide, wide), 1))).astype(BF16)
        ranks = dot((on[0] + on[1]).astype(BF16), before)
        base = (block_of((1, wide), 1) * cap).astype(F32)
        seats = [
            known[k : k + 1] * chunk + base + jnp.sum(on[k] * ranks, 0, keepdims=True)
            for k in range(2)
        ]
        inv = (known[6:7] + known[7:8]) + known[8:9]
        table = jnp.concatenate(
            [seats[0], seats[1], known[2:3], known[3:4], known[4:5], known[5:6], inv, inv], 0
        )
        rows_t[phase] = table
        cols_t[phase] = jnp.transpose(
            jnp.concatenate([table, jnp.zeros((lanes - 8, wide), F32)], 0)
        )
        with jax.named_scope("landed_wait"):
            for slot in slots_of(phase):
                rows_in(slot).wait_recv()
        scale = gain[:, pl.ds(pl.multiple_of(my_t * width, width), width)]
        normed[...] = (
            landed[first : first + slots].reshape(some, width).astype(F32)
            * cols_t[phase, :some, 6:7]
            * scale
        ).astype(BF16)

        def pick(member):
            spots = (iota((chunk, some), 0) + member * chunk).astype(F32)
            chosen = (spots == rows_t[phase, 0:1, :some]) | (spots == rows_t[phase, 1:2, :some])
            return dot(chosen.astype(F32).astype(BF16), normed[...]).astype(BF16)

        x[my_t, phase * members + my_e] = pick(my_e)

        def send_rows(step, carry):
            to = lax.rem(my_e + members - step, members)
            picked[phase * members + to] = pick(to)
            rows_to(phase * members + to, phase * members + my_e, to).start()
            return carry

        lax.fori_loop(1, members, send_rows, 0)
        if phase + UPFRONT < PHASES:
            for k in sends[phase + UPFRONT]:
                rows_out(k).start()

    def rows_to(there, here, to):
        return remote(
            picked.at[there], x.at[my_t, here], s2_send.at[there], s2_recv.at[here], e=to
        )

    def result_to(there, here, to):
        return remote(
            result.at[there], back.at[here], r_send.at[there], r_recv.at[here], e=to
        )

    def half(ref, src, c, n):
        part = ref.shape[3] // 2
        return ref.at[src, c, :, pl.ds(n * part, part)]

    def own_to(ref, send, recv, c, n):
        return remote(
            ref.at[my_t, c], ref.at[my_t, c], send.at[n, c], recv.at[n, c],
            tp=right if n == 0 else left,
        )

    def arrived(ref, send, recv, c, n):
        src = left if n == 0 else right
        return remote(
            ref.at[src, c], ref.at[src, c], send.at[n, c], recv.at[n, c],
            tp=right if n == 0 else left,
        )

    def pass_on(ref, send, recv, c, n):
        src = left if n == 0 else right
        return remote(
            half(ref, src, c, n), half(ref, src, c, n), send.at[2 + n, c], recv.at[2 + n, c],
            tp=right if n == 0 else left,
        )

    def passed(ref, send, recv, c, n):
        return remote(
            half(ref, across, c, n), half(ref, across, c, n), send.at[2 + n, c],
            recv.at[2 + n, c], tp=right if n == 0 else left,
        )

    def enter(i, off, phase, e, c):
        @pl.when(off > 0)
        def _():
            rows_to(c, c, e).wait_recv()

        for n in range(2):
            own_to(x, x_send, x_recv, c, n).start()

    def forward_x(i, off, phase, e, c):
        for n in range(2):
            arrived(x, x_send, x_recv, c, n).wait_recv()
            pass_on(x, x_send, x_recv, c, n).start()

    def widen(i, off, phase, e, c):
        for n in range(2):
            passed(x, x_send, x_recv, c, n).wait_recv()
        gate = jnp.zeros((chunk, ff), F32)
        up = jnp.zeros((chunk, ff), F32)
        for t in range(ways):
            piece = x[t, c]
            gate = gate + dot(piece, wg[t * width : (t + 1) * width])
            up = up + dot(piece, wu[t * width : (t + 1) * width])
        h[my_t, c] = (gate / (1.0 + jnp.exp(-gate)) * up).astype(BF16)
        for n in range(2):
            own_to(h, h_send, h_recv, c, n).start()

    def forward_h(i, off, phase, e, c):
        for n in range(2):
            arrived(h, h_send, h_recv, c, n).wait_recv()
            pass_on(h, h_send, h_recv, c, n).start()

    def narrow(i, off, phase, e, c):
        for n in range(2):
            passed(h, h_send, h_recv, c, n).wait_recv()
        made = jnp.zeros((chunk, width), F32)
        for t in range(ways):
            made = made + dot(h[t, c], wd[t * ff : (t + 1) * ff])

        @pl.when(off == 0)
        def _():
            back[c] = made.astype(BF16)

        @pl.when(off > 0)
        def _():
            result[c] = made.astype(BF16)
            result_to(c, phase * members + my_e, e).start()

    def mix(i, off, phase, e, c):
        j = lax.rem(my_e + members - off, members)
        there = phase * members + j

        @pl.when(off > 0)
        def _():
            result_to(there, there, j).wait_recv()

        spots = (iota((some, chunk), 1) + j * chunk).astype(F32)
        hit = [spots == cols_t[phase, :some, k : k + 1] for k in range(2)]
        part = jnp.zeros((some, width), F32)
        for n in range(2):
            share = jnp.where(
                hit[0],
                cols_t[phase, :some, 2 + n : 3 + n],
                jnp.where(hit[1], cols_t[phase, :some, 4 + n : 5 + n], 0.0),
            )
            part = part + dot(share.astype(BF16), back[there])

        @pl.when(off == 0)
        def _():
            total[...] = part

        @pl.when(off > 0)
        def _():
            total[...] += part

        for p in range(PHASES):
            @pl.when(i == (p + 1) * members - 1)
            def _():
                first = p * slots
                mixed[first : first + slots] = (
                    total[...].astype(BF16).reshape(slots, per_group, width)
                )
                for slot in slots_of(p):
                    home_out(slot).start()

    def stage(step, lag, name, body):
        with jax.named_scope(name):
            @pl.when((step >= lag) & (step < chunks + lag))
            def _():
                i = step - lag
                phase, off = i // members, lax.rem(i, members)
                e = lax.rem(my_e + off, members)
                body(i, off, phase, e, phase * members + e)

    def steps(step, carry):
        stage(step, LAGS[0], "enter", enter)
        stage(step, LAGS[1], "forward_x", forward_x)
        stage(step, LAGS[3], "forward_h", forward_h)
        stage(step, LAGS[2], "widen", widen)
        stage(step, LAGS[4], "narrow", narrow)
        stage(step, LAGS[5], "mix", mix)

        for p in range(1, PHASES):
            @pl.when(step == LEAD_AT[p - 1])
            def _():
                lead(p)

        return carry

    lead(0)
    lax.fori_loop(0, chunks + LAGS[5], steps, 0)
    home[my_g] = mixed[home_slot]
    unsort = (iota((rows, rows), 1).astype(F32) == place_col).astype(BF16)

    for copy in q1:
        copy.wait_send()
    for k in range(1, groups):
        rows_out(k).wait_send()
        facts_out(k).wait_send()

    def drain(step, carry):
        phase, off = step // members, lax.rem(step, members)

        @pl.when(off > 0)
        def _():
            e = lax.rem(my_e + off, members)
            rows_to(phase * members + e, phase * members + my_e, e).wait_send()
            result_to(phase * members + e, phase * members + my_e, e).wait_send()

        for n in range(2):
            own_to(x, x_send, x_recv, step, n).wait_send()
            pass_on(x, x_send, x_recv, step, n).wait_send()
            own_to(h, h_send, h_recv, step, n).wait_send()
            pass_on(h, h_send, h_recv, step, n).wait_send()
        return carry

    lax.fori_loop(0, chunks, drain, 0)
    with jax.named_scope("home_wait"):
        for k in range(1, groups):
            home_in(k).wait_recv()
    for phase in range(PHASES):
        for slot in slots_of(phase):
            home_out(slot).wait_send()
    out[...] = dot(unsort, home[...].reshape(rows, width)).astype(BF16)


def body(
    tokens,
    group_choice,
    expert_choice,
    group_weight,
    expert_weight,
    norm_gain,
    w_gate,
    w_up,
    w_down,
):
    rows, width = tokens.shape
    groups, members, ways = lax.axis_size("g"), lax.axis_size("e"), lax.axis_size("tp")
    per_group = rows // groups
    mean_load = 2 * per_group // members
    cap = mean_load + min(mean_load // 2, per_group - mean_load)
    chunk = groups // PHASES * cap
    chunks = PHASES * members
    some = rows // PHASES
    wide = -(-some // 128) * 128
    ff = w_gate.shape[2]
    dma = pltpu.SemaphoreType.DMA
    vmem = pl.BlockSpec(memory_space=pltpu.VMEM)
    hbm = pl.BlockSpec(memory_space=pltpu.HBM)
    return pl.pallas_call(
        functools.partial(kernel, groups, members, ways, per_group, cap),
        out_shape=jax.ShapeDtypeStruct((rows, width), BF16),
        in_specs=[hbm] + [vmem] * 5 + [hbm] * 3,
        out_specs=vmem,
        scratch_shapes=[
            pltpu.VMEM((rows, width), BF16),
            pltpu.VMEM((ways * width, ff), BF16),
            pltpu.VMEM((ways * width, ff), BF16),
            pltpu.VMEM((ways * ff, width), BF16),
            pltpu.VMEM((ways, 8, rows), F32),
            pltpu.VMEM((groups, per_group, width), BF16),
            pltpu.VMEM((groups, 16, 128), BF16),
            pltpu.VMEM((groups, per_group, width), BF16),
            pltpu.VMEM((groups, 16, 128), BF16),
            pltpu.VMEM((some, width), BF16),
            pltpu.VMEM((PHASES, 8, wide), F32),
            pltpu.VMEM((PHASES, wide, 128), F32),
            pltpu.VMEM((chunks, chunk, width), BF16),
            pltpu.VMEM((ways, chunks, chunk, width), BF16),
            pltpu.VMEM((ways, chunks, chunk, ff), BF16),
            pltpu.VMEM((chunks, chunk, width), BF16),
            pltpu.VMEM((chunks, chunk, width), BF16),
            pltpu.VMEM((some, width), F32),
            pltpu.VMEM((groups, per_group, width), BF16),
            pltpu.VMEM((groups, per_group, width), BF16),
            dma((4,)),
            dma((ways,)), dma((ways,)),
            dma((groups,)), dma((groups,)),
            dma((groups,)), dma((groups,)),
            dma((chunks,)), dma((chunks,)),
            dma((4, chunks)), dma((4, chunks)),
            dma((4, chunks)), dma((4, chunks)),
            dma((chunks,)), dma((chunks,)),
            dma((groups,)), dma((groups,)),
        ],
        compiler_params=pltpu.CompilerParams(
            collective_id=0, has_side_effects=True, vmem_limit_bytes=62 * 1024 * 1024
        ),
        name="expert_layer",
    )(
        tokens,
        group_choice[None, :],
        expert_choice.T,
        group_weight[None, :],
        expert_weight.T,
        norm_gain[None, :],
        w_gate[0],
        w_up[0],
        w_down[0],
    )


def solution(mesh):
    members = GROUP_SIZE
    split = Mesh(
        mesh.devices.reshape(
            mesh.shape["grp"], mesh.shape["ep"] // members, members, mesh.shape["tp"]
        ),
        ("grp", "g", "e", "tp"),
    )
    placed = (
        P(GRP_EP, "tp"),
        P(GRP_EP),
        P(GRP_EP, None),
        P(GRP_EP),
        P(GRP_EP, None),
        P(),
        P(EP, None, "tp"),
        P(EP, None, "tp"),
        P(EP, None, "tp"),
    )
    return jax.shard_map(
        body, mesh=split, in_specs=placed, out_specs=P(GRP_EP, "tp"), check_vma=False
    )
```

```python
import functools

import jax
import jax.numpy as jnp
from jax import lax
from jax.experimental import pallas as pl
from jax.experimental.pallas import tpu as pltpu
from jax.sharding import Mesh
from jax.sharding import PartitionSpec as P

GRP_EP = ("grp", "g", "e")
EP = ("g", "e")
GROUP_SIZE = 8
MESH = pl.DeviceIdType.MESH
F32 = jnp.float32
BF16 = jnp.bfloat16


def dot(a, b):
    return jnp.dot(a, b, preferred_element_type=F32)


def iota(shape, dim):
    return lax.broadcasted_iota(jnp.int32, shape, dim)


def pieces(x, count):
    parts = []
    for _ in range(count):
        part = x.astype(BF16)
        parts.append(part)
        x = x - part.astype(F32)
    return parts


def remote(src, dst, send, recv, **where):
    return pltpu.make_async_remote_copy(
        src_ref=src, dst_ref=dst, send_sem=send, recv_sem=recv,
        device_id=where, device_id_type=MESH,
    )


LAGS = (0, 2, 4, 7, 9, 13)
AWAY = (2, 4, 3, 1)
PHASES = 4
LEAD_AT = (6, 14, 22)
UPFRONT = 2


def kernel(
    groups, members, ways, per_group, cap,
    tok_hbm, grow, crow, gw, ew, gain, wg_hbm, wu_hbm, wd_hbm,
    out,
    tok, wg, wu, wd, sq, sorted_rows, facts, landed, facts_in, normed, rows_t, cols_t,
    picked, x, h, result, back, total, mixed, home,
    w_sem, q_send, q_recv, s1_send, s1_recv, m_send, m_recv, s2_send, s2_recv,
    x_send, x_recv, h_send, h_recv, r_send, r_recv, f_send, f_recv,
):
    my_g, my_e, my_t = lax.axis_index("g"), lax.axis_index("e"), lax.axis_index("tp")
    right, left = lax.rem(my_t + 1, ways), lax.rem(my_t + ways - 1, ways)
    across = lax.rem(my_t + 2, ways)
    rows, width = tok.shape
    slots = groups // PHASES
    some = rows // PHASES
    chunk = slots * cap
    chunks = PHASES * members
    ff = wg.shape[1]
    lanes = 128
    wide = -(-some // lanes) * lanes

    tok_load = pltpu.make_async_copy(tok_hbm, tok, w_sem.at[3])
    tok_load.start()
    loads = [
        pltpu.make_async_copy(src, dst, w_sem.at[n])
        for n, (src, dst) in enumerate(((wg_hbm, wg), (wu_hbm, wu), (wd_hbm, wd)))
    ]
    for load in loads:
        load.start()

    barrier = pltpu.get_barrier_semaphore()

    def greet(**where):
        pl.semaphore_signal(barrier, inc=1, device_id=where, device_id_type=MESH)

    near = members // 2
    home_slot = 2 * AWAY.index(near) + 1
    per_phase = len(AWAY) // PHASES
    sends = [
        sum([(a,) if a == near else (a, groups - a) for a in AWAY[n : n + per_phase]], ())
        for n in range(0, len(AWAY), per_phase)
    ]

    def slots_of(phase):
        every = range(groups // PHASES * phase, groups // PHASES * (phase + 1))
        return [slot for slot in every if slot != home_slot]

    my_part = my_e // near

    def leader_of(k):
        if k == near:
            return lax.rem(my_e + near, members)
        return (k // near) * near + lax.rem(my_e + k, near)

    def slot_there(k):
        if k == near:
            return home_slot - 1
        return 2 * AWAY.index(min(k, groups - k)) + my_part

    def source_of(slot):
        if slot == home_slot - 1:
            return near, lax.rem(my_e + near, members)
        away = AWAY[slot // 2]
        k = away + my_part * (groups - 2 * away)
        return k, lax.rem(my_e + groups - k, near) + (slot % 2) * near

    def back_by(k):
        return lax.rem(my_g + groups - k, groups)

    for k in range(1, groups):
        greet(g=lax.rem(my_g + k, groups), e=leader_of(k))
    for phase in range(PHASES):
        for slot in slots_of(phase):
            k, e = source_of(slot)
            greet(g=back_by(k), e=e)
    for off in range(1, members):
        greet(e=lax.rem(my_e + off, members))
    for off in range(1, ways):
        greet(tp=lax.rem(my_t + off, ways))

    earlier = iota((rows, rows), 0) < iota((rows, rows), 1)
    marks = (grow[...] == iota((groups, rows), 0)).astype(F32)
    rank_row = jnp.sum(dot(marks.astype(BF16), earlier.astype(BF16)) * marks, 0, keepdims=True)
    place_row = grow[...] * per_group + rank_row.astype(jnp.int32)
    sort = (iota((rows, rows), 0) == place_row).astype(BF16)
    two = jnp.concatenate(
        [place_row.astype(F32), grow[...] * lanes + rank_row, jnp.zeros((lanes - 2, rows), F32)], 0
    )
    place_cols = jnp.transpose(two)
    place_col, place_wide = place_cols[:, 0:1], place_cols[:, 1:2]
    tok_load.wait()
    sorted_rows[...] = dot(sort, tok[...]).astype(BF16).reshape(groups, per_group, width)
    values = tok[...].astype(F32)
    squares = jnp.sum(values * values, -1, keepdims=True)
    squares = jnp.transpose(jnp.broadcast_to(squares, (rows, lanes)))
    sq[my_t] = squares[:8]

    with jax.named_scope("barrier_wait"):
        pl.semaphore_wait(barrier, 2 * groups + members + ways - 4)

    def rows_out(k):
        to = lax.rem(my_g + k, groups)
        slot = slot_there(k)
        return remote(
            sorted_rows.at[to], landed.at[slot], s1_send.at[k], s1_recv.at[slot],
            g=to, e=leader_of(k),
        )

    def rows_in(slot):
        k, e = source_of(slot)
        return remote(
            sorted_rows.at[slot], landed.at[slot], s1_send.at[slot], s1_recv.at[slot],
            g=back_by(k), e=e,
        )

    def facts_out(k):
        to = lax.rem(my_g + k, groups)
        slot = slot_there(k)
        return remote(
            facts.at[to], facts_in.at[slot], m_send.at[k], m_recv.at[slot],
            g=to, e=leader_of(k),
        )

    def facts_to_me(slot):
        k, e = source_of(slot)
        return remote(
            facts.at[slot], facts_in.at[slot], m_send.at[slot], m_recv.at[slot],
            g=back_by(k), e=e,
        )

    def home_out(slot):
        k, e = source_of(slot)
        return remote(
            mixed.at[slot], home.at[my_g], f_send.at[slot], f_recv.at[k], g=back_by(k), e=e
        )

    def home_in(k):
        src = lax.rem(my_g + k, groups)
        return remote(
            mixed.at[k], home.at[src], f_send.at[k], f_recv.at[k], g=src, e=leader_of(k)
        )

    q1 = []
    for off in range(1, ways):
        to = lax.rem(my_t + off, ways)
        q1.append(remote(sq.at[my_t], sq.at[my_t], q_send.at[to], q_recv.at[my_t], tp=to))
        q1[-1].start()
    for k in sum(sends[:UPFRONT], ()):
        rows_out(k).start()
    landed[home_slot] = sorted_rows[my_g]

    spread = (iota((rows, groups * lanes), 1).astype(F32) == place_wide).astype(BF16)
    with jax.named_scope("sq_wait"):
        for off in range(1, ways):
            src = lax.rem(my_t + off, ways)
            remote(sq.at[src], sq.at[src], q_send.at[src], q_recv.at[src], tp=src).wait_recv()
    model_width = width * ways
    all_squares = jnp.sum(sq[...], 0)[:1]
    inv_rms = lax.rsqrt(all_squares / model_width + 1e-06)
    weights = ew[...]
    mixing = gw[...] * weights / jnp.sum(weights, 0, keepdims=True)
    choice = crow[...].astype(F32)
    fields = [choice[0:1], choice[1:2]]
    for k in range(2):
        fields += [p.astype(F32) for p in pieces(mixing[k : k + 1], 2)]
    fields += [p.astype(F32) for p in pieces(inv_rms, 3)]
    fields.append(jnp.zeros((16 - len(fields), rows), F32))
    fields = jnp.concatenate(fields, 0).astype(BF16)
    spread_fields = dot(fields, spread).astype(BF16)
    for n in range(groups):
        facts[n] = spread_fields[:, n * lanes : (n + 1) * lanes]
    for k in sum(sends, ()):
        facts_out(k).start()
    facts_in[home_slot] = facts[my_g]
    for load in loads:
        load.wait()

    def block_of(shape, dim):
        spot = iota(shape, dim)
        block = jnp.zeros(shape, jnp.int32)
        for n in range(1, slots):
            block = block + (spot >= n * per_group).astype(jnp.int32)
        return block

    def lead(phase):
        first = phase * slots
        with jax.named_scope("facts_wait"):
            for slot in slots_of(phase):
                facts_to_me(slot).wait_recv()
        known = jnp.zeros((16, wide), F32)
        for n in range(slots):
            shift = (iota((lanes, wide), 0) + n * per_group == iota((lanes, wide), 1)).astype(BF16)
            known = known + dot(facts_in[first + n], shift)
        kinds = iota((members, wide), 0).astype(F32)
        on = [(known[k : k + 1] == kinds).astype(F32) for k in range(2)]
        same = block_of((wide, 1), 0) == block_of((1, wide), 1)
        before = (same & (iota((wide, wide), 0) < iota((wide, wide), 1))).astype(BF16)
        ranks = dot((on[0] + on[1]).astype(BF16), before)
        base = (block_of((1, wide), 1) * cap).astype(F32)
        seats = [
            known[k : k + 1] * chunk + base + jnp.sum(on[k] * ranks, 0, keepdims=True)
            for k in range(2)
        ]
        inv = (known[6:7] + known[7:8]) + known[8:9]
        table = jnp.concatenate(
            [seats[0], seats[1], known[2:3], known[3:4], known[4:5], known[5:6], inv, inv], 0
        )
        rows_t[phase] = table
        cols_t[phase] = jnp.transpose(
            jnp.concatenate([table, jnp.zeros((lanes - 8, wide), F32)], 0)
        )
        with jax.named_scope("landed_wait"):
            for slot in slots_of(phase):
                rows_in(slot).wait_recv()
        scale = gain[:, pl.ds(pl.multiple_of(my_t * width, width), width)]
        normed[...] = (
            landed[first : first + slots].reshape(some, width).astype(F32)
            * cols_t[phase, :some, 6:7]
            * scale
        ).astype(BF16)

        def pick(member):
            spots = (iota((chunk, some), 0) + member * chunk).astype(F32)
            chosen = (spots == rows_t[phase, 0:1, :some]) | (spots == rows_t[phase, 1:2, :some])
            return dot(chosen.astype(F32).astype(BF16), normed[...]).astype(BF16)

        x[my_t, phase * members + my_e] = pick(my_e)

        def send_rows(step, carry):
            to = lax.rem(my_e + members - step, members)
            picked[phase * members + to] = pick(to)
            rows_to(phase * members + to, phase * members + my_e, to).start()
            return carry

        lax.fori_loop(1, members, send_rows, 0)
        if phase + UPFRONT < PHASES:
            for k in sends[phase + UPFRONT]:
                rows_out(k).start()

    def rows_to(there, here, to):
        return remote(
            picked.at[there], x.at[my_t, here], s2_send.at[there], s2_recv.at[here], e=to
        )

    def result_to(there, here, to):
        return remote(
            result.at[there], back.at[here], r_send.at[there], r_recv.at[here], e=to
        )

    def half(ref, src, c, n):
        part = ref.shape[3] // 2
        return ref.at[src, c, :, pl.ds(n * part, part)]

    def own_to(ref, send, recv, c, n):
        return remote(
            ref.at[my_t, c], ref.at[my_t, c], send.at[n, c], recv.at[n, c],
            tp=right if n == 0 else left,
        )

    def arrived(ref, send, recv, c, n):
        src = left if n == 0 else right
        return remote(
            ref.at[src, c], ref.at[src, c], send.at[n, c], recv.at[n, c],
            tp=right if n == 0 else left,
        )

    def pass_on(ref, send, recv, c, n):
        src = left if n == 0 else right
        return remote(
            half(ref, src, c, n), half(ref, src, c, n), send.at[2 + n, c], recv.at[2 + n, c],
            tp=right if n == 0 else left,
        )

    def passed(ref, send, recv, c, n):
        return remote(
            half(ref, across, c, n), half(ref, across, c, n), send.at[2 + n, c],
            recv.at[2 + n, c], tp=right if n == 0 else left,
        )

    def enter(i, off, phase, e, c):
        @pl.when(off > 0)
        def _():
            rows_to(c, c, e).wait_recv()

        for n in range(2):
            own_to(x, x_send, x_recv, c, n).start()

    def forward_x(i, off, phase, e, c):
        for n in range(2):
            arrived(x, x_send, x_recv, c, n).wait_recv()
            pass_on(x, x_send, x_recv, c, n).start()

    def widen(i, off, phase, e, c):
        for n in range(2):
            passed(x, x_send, x_recv, c, n).wait_recv()
        gate = jnp.zeros((chunk, ff), F32)
        up = jnp.zeros((chunk, ff), F32)
        for t in range(ways):
            piece = x[t, c]
            gate = gate + dot(piece, wg[t * width : (t + 1) * width])
            up = up + dot(piece, wu[t * width : (t + 1) * width])
        h[my_t, c] = (gate / (1.0 + jnp.exp(-gate)) * up).astype(BF16)
        for n in range(2):
            own_to(h, h_send, h_recv, c, n).start()

    def forward_h(i, off, phase, e, c):
        for n in range(2):
            arrived(h, h_send, h_recv, c, n).wait_recv()
            pass_on(h, h_send, h_recv, c, n).start()

    def narrow(i, off, phase, e, c):
        for n in range(2):
            passed(h, h_send, h_recv, c, n).wait_recv()
        made = jnp.zeros((chunk, width), F32)
        for t in range(ways):
            made = made + dot(h[t, c], wd[t * ff : (t + 1) * ff])

        @pl.when(off == 0)
        def _():
            back[c] = made.astype(BF16)

        @pl.when(off > 0)
        def _():
            result[c] = made.astype(BF16)
            result_to(c, phase * members + my_e, e).start()

    def mix(i, off, phase, e, c):
        j = lax.rem(my_e + members - off, members)
        there = phase * members + j

        @pl.when(off > 0)
        def _():
            result_to(there, there, j).wait_recv()

        spots = (iota((some, chunk), 1) + j * chunk).astype(F32)
        hit = [spots == cols_t[phase, :some, k : k + 1] for k in range(2)]
        part = jnp.zeros((some, width), F32)
        for n in range(2):
            share = jnp.where(
                hit[0],
                cols_t[phase, :some, 2 + n : 3 + n],
                jnp.where(hit[1], cols_t[phase, :some, 4 + n : 5 + n], 0.0),
            )
            part = part + dot(share.astype(BF16), back[there])

        @pl.when(off == 0)
        def _():
            total[...] = part

        @pl.when(off > 0)
        def _():
            total[...] += part

        for p in range(PHASES):
            @pl.when(i == (p + 1) * members - 1)
            def _():
                first = p * slots
                mixed[first : first + slots] = (
                    total[...].astype(BF16).reshape(slots, per_group, width)
                )
                for slot in slots_of(p):
                    home_out(slot).start()

    def stage(step, lag, name, body):
        with jax.named_scope(name):
            @pl.when((step >= lag) & (step < chunks + lag))
            def _():
                i = step - lag
                phase, off = i // members, lax.rem(i, members)
                e = lax.rem(my_e + off, members)
                body(i, off, phase, e, phase * members + e)

    def steps(step, carry):
        stage(step, LAGS[0], "enter", enter)
        stage(step, LAGS[1], "forward_x", forward_x)
        stage(step, LAGS[3], "forward_h", forward_h)
        stage(step, LAGS[2], "widen", widen)
        stage(step, LAGS[4], "narrow", narrow)
        stage(step, LAGS[5], "mix", mix)

        for p in range(1, PHASES):
            @pl.when(step == LEAD_AT[p - 1])
            def _():
                lead(p)

        return carry

    lead(0)
    lax.fori_loop(0, chunks + LAGS[5], steps, 0)
    home[my_g] = mixed[home_slot]
    unsort = (iota((rows, rows), 1).astype(F32) == place_col).astype(BF16)

    for copy in q1:
        copy.wait_send()
    for k in range(1, groups):
        rows_out(k).wait_send()
        facts_out(k).wait_send()

    def drain(step, carry):
        phase, off = step // members, lax.rem(step, members)

        @pl.when(off > 0)
        def _():
            e = lax.rem(my_e + off, members)
            rows_to(phase * members + e, phase * members + my_e, e).wait_send()
            result_to(phase * members + e, phase * members + my_e, e).wait_send()

        for n in range(2):
            own_to(x, x_send, x_recv, step, n).wait_send()
            pass_on(x, x_send, x_recv, step, n).wait_send()
            own_to(h, h_send, h_recv, step, n).wait_send()
            pass_on(h, h_send, h_recv, step, n).wait_send()
        return carry

    lax.fori_loop(0, chunks, drain, 0)
    with jax.named_scope("home_wait"):
        for k in range(1, groups):
            home_in(k).wait_recv()
    for phase in range(PHASES):
        for slot in slots_of(phase):
            home_out(slot).wait_send()
    out[...] = dot(unsort, home[...].reshape(rows, width)).astype(BF16)


def body(
    tokens,
    group_choice,
    expert_choice,
    group_weight,
    expert_weight,
    norm_gain,
    w_gate,
    w_up,
    w_down,
):
    rows, width = tokens.shape
    groups, members, ways = lax.axis_size("g"), lax.axis_size("e"), lax.axis_size("tp")
    per_group = rows // groups
    mean_load = 2 * per_group // members
    cap = mean_load + min(mean_load // 2, per_group - mean_load)
    chunk = groups // PHASES * cap
    chunks = PHASES * members
    some = rows // PHASES
    wide = -(-some // 128) * 128
    ff = w_gate.shape[2]
    dma = pltpu.SemaphoreType.DMA
    vmem = pl.BlockSpec(memory_space=pltpu.VMEM)
    hbm = pl.BlockSpec(memory_space=pltpu.HBM)
    return pl.pallas_call(
        functools.partial(kernel, groups, members, ways, per_group, cap),
        out_shape=jax.ShapeDtypeStruct((rows, width), BF16),
        in_specs=[hbm] + [vmem] * 5 + [hbm] * 3,
        out_specs=vmem,
        scratch_shapes=[
            pltpu.VMEM((rows, width), BF16),
            pltpu.VMEM((ways * width, ff), BF16),
            pltpu.VMEM((ways * width, ff), BF16),
            pltpu.VMEM((ways * ff, width), BF16),
            pltpu.VMEM((ways, 8, rows), F32),
            pltpu.VMEM((groups, per_group, width), BF16),
            pltpu.VMEM((groups, 16, 128), BF16),
            pltpu.VMEM((groups, per_group, width), BF16),
            pltpu.VMEM((groups, 16, 128), BF16),
            pltpu.VMEM((some, width), BF16),
            pltpu.VMEM((PHASES, 8, wide), F32),
            pltpu.VMEM((PHASES, wide, 128), F32),
            pltpu.VMEM((chunks, chunk, width), BF16),
            pltpu.VMEM((ways, chunks, chunk, width), BF16),
            pltpu.VMEM((ways, chunks, chunk, ff), BF16),
            pltpu.VMEM((chunks, chunk, width), BF16),
            pltpu.VMEM((chunks, chunk, width), BF16),
            pltpu.VMEM((some, width), F32),
            pltpu.VMEM((groups, per_group, width), BF16),
            pltpu.VMEM((groups, per_group, width), BF16),
            dma((4,)),
            dma((ways,)), dma((ways,)),
            dma((groups,)), dma((groups,)),
            dma((groups,)), dma((groups,)),
            dma((chunks,)), dma((chunks,)),
            dma((4, chunks)), dma((4, chunks)),
            dma((4, chunks)), dma((4, chunks)),
            dma((chunks,)), dma((chunks,)),
            dma((groups,)), dma((groups,)),
        ],
        compiler_params=pltpu.CompilerParams(
            collective_id=0, has_side_effects=True, vmem_limit_bytes=62 * 1024 * 1024
        ),
        name="expert_layer",
    )(
        tokens,
        group_choice[None, :],
        expert_choice.T,
        group_weight[None, :],
        expert_weight.T,
        norm_gain[None, :],
        w_gate[0],
        w_up[0],
        w_down[0],
    )


def solution(mesh):
    members = GROUP_SIZE
    split = Mesh(
        mesh.devices.reshape(
            mesh.shape["grp"], mesh.shape["ep"] // members, members, mesh.shape["tp"]
        ),
        ("grp", "g", "e", "tp"),
    )
    placed = (
        P(GRP_EP, "tp"),
        P(GRP_EP),
        P(GRP_EP, None),
        P(GRP_EP),
        P(GRP_EP, None),
        P(),
        P(EP, None, "tp"),
        P(EP, None, "tp"),
        P(EP, None, "tp"),
    )
    return jax.shard_map(
        body, mesh=split, in_specs=placed, out_specs=P(GRP_EP, "tp"), check_vma=False
    )
```
